32 devices in a mesh: sp: 8 (over z, x), dp: 4 (over y, core).
Axes of the slice: x: 2, y: 2, z: 4, core: 2. Of those that a mesh axis runs over, the one named last changes fastest.
Arguments:
- queries: bfloat16 [4, 1024, 16, 128], P('dp', 'sp'), may hold values from -3.5 to 2
- key_rows: bfloat16 [4, 1024, 16, 128], P('dp', 'sp'), may hold values from -4 to 5.3
- values: bfloat16 [4, 1024, 16, 128], P('dp', 'sp'), may hold values from -6 to 6
- residual: bfloat16 [4, 1024, 4096], P('dp', 'sp'), may hold values from -6 to 6
- out_weight: bfloat16 [2048, 4096], P(None, 'dp'), may hold values from -0.125 to 0.125
- mixer_gain: float32 [4096], replicated, may hold values from 0.1 to 1.9
- expert_gain: float32 [4096], replicated, may hold values from 0.1 to 1.9
- gate_weight: bfloat16 [32, 4096, 512], P(('sp', 'dp')), may hold values from -0.09375 to 0.09375
- up_weight: bfloat16 [32, 4096, 512], P(('sp', 'dp')), may hold values from -0.09375 to 0.09375
- expert_down_matrix: bfloat16 [32, 512, 4096], P(('sp', 'dp')), may hold values from -0.25 to 0.25
- routes: int32 [4, 1024, 2], P('dp', 'sp'), may hold values from 0 to 31, all different within a row; in each aligned block of 128 rows (0 to 127, 128 to 255, ..., all dimensions but the last counted through in order) at most 12 rows name the same one
- route_weight: float32 [4, 1024, 2], P('dp', 'sp'), may hold values from 0.1 to 1
- output_gain: float32 [4096], replicated, may hold values from 0.1 to 1.9
Outputs:
- output: bfloat16 [4, 1024, 4096], P('dp', 'sp')
The draws below stay inside these ranges and needn't reach their ends.
Inputs may be any that keep to these rules, and one draw needn't show every extreme that they name: `routes`: each row names 2 different experts. Among the rows of one device no expert is named more than 12 times, and in every draw some device names some expert exactly 12 times.
All inputs are finite; a program needn't handle non-finite values.
Results may differ from the reference program's by a relative error of at most 0.009.
Values may be sent and summed in bfloat16 or wider, within the bound.
A program may use at most 192 MiB of HBM per device.

```python
import math
import jax
import jax.numpy as jnp
import numpy as np
from jax import lax

D = 4096
HEADS = 16
HD = 128
FF = 512
TOP = 2
SEG_DEV = 128
BATCH_SEQUENCES = 4
SEQUENCE_LENGTH = 1024
EXPERTS = 32
CAP = 12
N_SP = 8
N_DP = 4


def draw_queries(key, part):
    head_key = jax.random.fold_in(key, 11)
    noise_key = jax.random.fold_in(key, 12)
    spread_key = jax.random.fold_in(key, 13)
    shape = (BATCH_SEQUENCES, SEQUENCE_LENGTH, HEADS, HD)
    slow_level = (math.log(SEQUENCE_LENGTH) + 0.5) / math.sqrt(HD)
    fast_level = (math.log(40.0) + 0.5) / math.sqrt(HD)
    fast_heads = jax.random.uniform(head_key, (HEADS,), jnp.float32) < 0.5
    noise = 0.5 * jax.random.truncated_normal(noise_key, -4.0, 4.0, shape, jnp.float32)
    spread = jax.random.uniform(spread_key, (HEADS,), jnp.float32, 0.9, 1.1)
    tier_value = -jnp.where(fast_heads, fast_level, slow_level) * spread
    return (noise + tier_value[None, None, :, None]).astype(jnp.bfloat16)


def draw_key_rows(key, part):
    noise_key = jax.random.fold_in(key, 21)
    level_key = jax.random.fold_in(key, 22)
    spike_random_key = jax.random.fold_in(key, 23)
    shape = (BATCH_SEQUENCES, SEQUENCE_LENGTH, HEADS, HD)
    blocks = SEQUENCE_LENGTH // SEG_DEV
    noise = jax.random.truncated_normal(noise_key, -4.0, 4.0, shape, jnp.float32)
    tier_value = jnp.exp(jax.random.uniform(level_key, (BATCH_SEQUENCES, blocks), jnp.float32, math.log(0.85), math.log(1.18)))
    tier_value = jnp.repeat(tier_value, SEG_DEV, axis=1)
    sudden_spike = jax.random.uniform(spike_random_key, (BATCH_SEQUENCES, SEQUENCE_LENGTH), jnp.float32) < 6.0 / SEQUENCE_LENGTH
    tier_value = jnp.where(sudden_spike, 0.1, tier_value)
    return (noise + tier_value[:, :, None, None]).astype(jnp.bfloat16)


def shard_levels(stream_key, shape, shards, smallest, largest):
    level, own = 1.0, jax.random.fold_in(stream_key, 6)
    for position, blocks in shards:
        steps = jnp.exp(jax.random.uniform(jax.random.fold_in(own, position), (blocks,), jnp.float32, smallest / len(shards), largest / len(shards)))
        level = level * jnp.repeat(steps, shape[position] // blocks).reshape([-1 if axis == position else 1 for axis in range(len(shape))])
    return level


def shared_out(stream_key, own, number, rows, count, top, limit, lean):
    order = jax.random.permutation(stream_key, count)
    heavy_load, common = load_shares(count, rows * top, limit, lean, True), load_shares(count, rows * top, limit, lean, False)
    places = jnp.arange(count)

    def named(lengths, turn):
        used = int((lengths > 0).sum())
        fixed = max(1, used // 4)
        shifted = fixed + (places - fixed + turn * (used - fixed)) % max(1, count - fixed)
        return jnp.zeros((count,), jnp.int32).at[order[jnp.where(places < fixed, places, shifted)]].set(jnp.asarray(lengths, jnp.int32))

    lengths = jnp.where(number % 4 == 0, named(heavy_load, number // 4), named(common, number - number // 4 - 1))
    mixed = jax.random.permutation(jax.random.fold_in(own, 3), count)
    source_of, taker = mixed[0:count // 2 * 2:2], mixed[1:count // 2 * 2:2]
    margin = jnp.minimum(lengths[source_of] - 1, limit - lengths[taker]) // 2
    margin = jnp.where((source_of == order[0]) | (taker == order[0]) | (lengths[taker] == 0), 0, jnp.maximum(margin, 0))
    shifted = jax.random.randint(jax.random.fold_in(own, 4), (count // 2,), 0, 1 << 20) % (margin + 1)
    lengths = lengths.at[source_of].add(-shifted).at[taker].add(shifted)
    members = jnp.searchsorted(jnp.cumsum(lengths), jnp.arange(rows * top), side="right").astype(jnp.int32)
    grid = members.reshape(top, rows).T
    grid = grid[jax.random.permutation(jax.random.fold_in(own, 1), rows)]
    turn = jax.random.randint(jax.random.fold_in(own, 2), (rows, 1), 0, top)
    return jnp.take_along_axis(grid, (jnp.arange(top)[None, :] + turn) % top, axis=1)


def load_shares(count, total, reach, slope, full):
    weights = [(1 << 20) // math.isqrt(grade ** slope) + 1 for grade in range(1, count + 1)]
    largest = reach if full else min(reach, max(-(-total // count), total * weights[0] // sum(weights)))
    least = 1 if total - largest >= count - 1 else 0
    given, rest = [largest] + [least] * (count - 1), total - largest - least * (count - 1)
    while rest > 0:
        free = [i for i in range(1, count) if given[i] < largest] or [i for i in range(1, count) if given[i] < reach]
        whole, remaining = sum([weights[i] for i in free]), rest
        for i in free:
            addition = min(reach - given[i], max(1, remaining * weights[i] // whole), rest)
            given[i] = given[i] + addition
            rest = rest - addition
    return np.array(given)


def bell_draw(own_key, dims, deviation, bound, shards=(), held_as=jnp.bfloat16):
    loudness = shard_levels(own_key, dims, shards, -0.22, 0.18) if shards else 1.0
    array = jax.random.normal(own_key, dims, jnp.float32) * deviation * loudness
    return jnp.minimum(jnp.maximum(array, -bound), bound).astype(held_as)


def setup_inputs(seed: int = 0) -> dict:
    keys = jax.random.split(jax.random.key(seed), 14)
    queries = draw_queries(jax.random.fold_in(keys[13], 71), 0)
    key_rows = draw_key_rows(jax.random.fold_in(keys[13], 71), 0)
    values = bell_draw(keys[2], (BATCH_SEQUENCES, SEQUENCE_LENGTH, HEADS, HD), 1.0, 6.0, ((0, 4), (1, 8)))
    residual = bell_draw(keys[3], (BATCH_SEQUENCES, SEQUENCE_LENGTH, D), 1.0, 6.0, ((0, 4), (1, 8)))
    out_weight = bell_draw(keys[4], (HEADS * HD, D), (HEADS * HD) ** -0.5, 0.125, ((1, 4),))
    mixer_gain = jnp.clip(1.0 + 0.18 * jax.random.normal(keys[5], (D,), jnp.float32), 0.1, 1.9)
    expert_gain = jnp.clip(1.0 + 0.18 * jax.random.normal(keys[6], (D,), jnp.float32), 0.1, 1.9)
    gate_weight = bell_draw(keys[7], (EXPERTS, D, FF), D ** -0.5, 0.09375, ((0, 32),))
    up_weight = bell_draw(keys[8], (EXPERTS, D, FF), D ** -0.5, 0.09375, ((0, 32),))
    expert_down_matrix = bell_draw(keys[9], (EXPERTS, FF, D), FF ** -0.5, 0.25, ((0, 32),))
    routes_keys = jax.random.split(jax.random.fold_in(keys[10], 1), BATCH_SEQUENCES * SEQUENCE_LENGTH // SEG_DEV)
    routes_turns = jax.random.permutation(jax.random.fold_in(keys[10], 3), BATCH_SEQUENCES * SEQUENCE_LENGTH // SEG_DEV)
    routes = jax.vmap(lambda own, number: shared_out(jax.random.fold_in(keys[10], 2), own, number, SEG_DEV, EXPERTS, TOP, CAP, 2))(routes_keys, routes_turns).reshape((BATCH_SEQUENCES, SEQUENCE_LENGTH, TOP))
    route_weight = jnp.clip(0.1 + 0.9 * jax.random.uniform(keys[11], (BATCH_SEQUENCES, SEQUENCE_LENGTH, TOP), jnp.float32) ** shard_levels(keys[11], (BATCH_SEQUENCES, SEQUENCE_LENGTH, TOP), ((0, 4), (1, 8)), -0.2, 0.2), 0.1, 1.0)
    output_gain = jnp.clip(1.0 + 0.18 * jax.random.normal(keys[12], (D,), jnp.float32), 0.1, 1.9)
    return dict(queries=queries, key_rows=key_rows, values=values, residual=residual, out_weight=out_weight, mixer_gain=mixer_gain, expert_gain=expert_gain, gate_weight=gate_weight, up_weight=up_weight, expert_down_matrix=expert_down_matrix, routes=routes, route_weight=route_weight, output_gain=output_gain)


EPSILON = 1e-06

def normed_token_rows(matrix, gain):
    return matrix * lax.rsqrt(lax.optimization_barrier(jnp.mean(matrix * matrix, axis=-1, keepdims=True)) + EPSILON) * gain

def stick_head(query_rows, key_part, value_part):
    length = query_rows.shape[0]
    block_rows = min(512, length)
    score_scale = HD ** (-0.5)
    pieces = []
    for block_index in range(length // block_rows):
        row_start = block_index * block_rows
        row_stop = row_start + block_rows
        scores = jnp.dot(query_rows[row_start:row_stop], key_part[:row_stop].T, preferred_element_type=jnp.float32) * score_scale
        key_pos = lax.broadcasted_iota(jnp.int32, (block_rows, row_stop), 1)
        query_pos = lax.broadcasted_iota(jnp.int32, (block_rows, row_stop), 0) + row_start
        is_past = key_pos < query_pos
        log_keep = jnp.where(is_past, -jax.nn.softplus(scores), jnp.float32(0.0))
        suffix = lax.cumsum(log_keep, axis=1, reverse=True) - log_keep
        weights = jnp.where(is_past, jnp.exp(jax.nn.log_sigmoid(scores) + suffix), jnp.float32(0.0)).astype(jnp.bfloat16)
        pieces.append(jnp.dot(weights, value_part[:row_stop], preferred_element_type=jnp.float32).astype(jnp.bfloat16))
    return jnp.concatenate(pieces, axis=0)

def reference(queries, key_rows, values, residual, out_weight, mixer_gain, expert_gain, gate_weight, up_weight, expert_down_matrix, routes, route_weight, output_gain):

    def by_head(tensor):
        return jnp.transpose(tensor, (0, 2, 1, 3)).reshape(BATCH_SEQUENCES * HEADS, SEQUENCE_LENGTH, HD)

    def per_pair(operands):
        return stick_head(operands[0], operands[1], operands[2])
    attended = lax.map(per_pair, (by_head(queries), by_head(key_rows), by_head(values)))
    attended = attended.reshape(BATCH_SEQUENCES, HEADS, SEQUENCE_LENGTH, HD).transpose(0, 2, 1, 3).reshape(BATCH_SEQUENCES, SEQUENCE_LENGTH, HEADS * HD)

    def token_side(operands):
        attn_rows, resid_rows = operands
        projected = jnp.dot(attn_rows, out_weight, preferred_element_type=jnp.float32)
        stream = (resid_rows.astype(jnp.float32) + normed_token_rows(projected, mixer_gain)).astype(jnp.bfloat16)
        expert_in = normed_token_rows(stream.astype(jnp.float32), expert_gain).astype(jnp.bfloat16)
        return (stream, expert_in)
    stream, expert_in = lax.map(token_side, (attended, residual))
    tokens = BATCH_SEQUENCES * SEQUENCE_LENGTH
    sources = N_SP * N_DP
    picked_experts = routes.reshape(BATCH_SEQUENCES, N_SP, SEG_DEV * TOP).astype(jnp.int32)
    onehot = (picked_experts[..., None] == jnp.arange(EXPERTS, dtype=jnp.int32)).astype(jnp.int32)
    before = jnp.cumsum(onehot, axis=2) - onehot
    slot_rank = lax.optimization_barrier(jnp.sum(before * onehot, axis=3)).astype(jnp.int32)
    source_id = jnp.arange(N_SP, dtype=jnp.int32)[None, :, None] * N_DP + jnp.arange(BATCH_SEQUENCES, dtype=jnp.int32)[:, None, None]
    token_id = jnp.arange(BATCH_SEQUENCES, dtype=jnp.int32)[:, None, None] * SEQUENCE_LENGTH + jnp.arange(N_SP, dtype=jnp.int32)[None, :, None] * SEG_DEV + jnp.arange(SEG_DEV * TOP, dtype=jnp.int32)[None, None, :] // TOP
    token_id = jnp.broadcast_to(token_id, picked_experts.shape).reshape(-1)
    dest_slot = (source_id * CAP + slot_rank).reshape(-1).astype(jnp.int32)
    expert_flat = picked_experts.reshape(-1)
    expert_slot_tokens = jnp.full((EXPERTS, sources * CAP), tokens, jnp.int32).at[expert_flat, dest_slot].set(token_id)
    padded = jnp.concatenate([expert_in.reshape(tokens, D), jnp.zeros((1, D), jnp.bfloat16)], axis=0)

    def per_expert(operands):
        token_list, gate_part, up_part, down_part = operands
        flat_rows = jnp.take(padded, token_list, axis=0)
        gate_out = jnp.dot(flat_rows, gate_part, preferred_element_type=jnp.float32)
        upward = jnp.dot(flat_rows, up_part, preferred_element_type=jnp.float32)
        hidden = (jax.nn.silu(gate_out) * upward).astype(jnp.bfloat16)
        return jnp.dot(hidden, down_part, preferred_element_type=jnp.float32).astype(jnp.bfloat16)
    served = lax.map(per_expert, (expert_slot_tokens, gate_weight, up_weight, expert_down_matrix))
    gathered = served[expert_flat, dest_slot]
    order = jnp.argsort(token_id * TOP + jnp.arange(tokens * TOP, dtype=jnp.int32) % TOP)
    gathered = gathered[order].reshape(tokens, TOP, D)
    combined = lax.optimization_barrier(jnp.sum(gathered.astype(jnp.float32) * route_weight.reshape(tokens, TOP)[:, :, None], axis=1))
    output = (stream.reshape(tokens, D).astype(jnp.float32) + normed_token_rows(combined, output_gain)).astype(jnp.bfloat16)
    return output.reshape(BATCH_SEQUENCES, SEQUENCE_LENGTH, D)
```

```python
import functools

import jax
import jax.numpy as jnp
from jax import lax
from jax.experimental import pallas as pl
from jax.experimental.pallas import tpu as pltpu
from jax.sharding import PartitionSpec as P

EPSILON = 1e-06
MESH = pl.DeviceIdType.MESH
VMEM_LIMIT = 56 * 1024 * 1024


def normed_token_rows(matrix, gain):
    return matrix * lax.rsqrt(jnp.mean(matrix * matrix, axis=-1, keepdims=True) + EPSILON) * gain


def peer_id(axes, sizes, flat):
    if len(axes) == 1:
        return {axes[0]: flat}
    return {axes[0]: lax.div(flat, sizes[1]), axes[1]: lax.rem(flat, sizes[1])}


def exchange_kernel(axes, sizes, n, count, *refs):
    ins, outs = refs[:count], refs[count : 2 * count]
    stages = refs[2 * count : 3 * count]
    send_sem, recv_sem, local_sem = refs[3 * count :]
    me = lax.axis_index(axes[0])
    if len(axes) == 2:
        me = me * sizes[1] + lax.axis_index(axes[1])

    barrier = pltpu.get_barrier_semaphore()

    def greet(k, carry):
        pl.semaphore_signal(
            barrier, inc=1, device_id=peer_id(axes, sizes, lax.rem(me + k, n)), device_id_type=MESH
        )
        return carry

    lax.fori_loop(1, n, greet, 0)
    loads = [
        pltpu.make_async_copy(ins[a].at[me], stages[a], local_sem.at[a]) for a in range(count)
    ]
    for load in loads:
        load.start()
    pl.semaphore_wait(barrier, n - 1)

    def copies(k):
        target = lax.rem(me + k, n)
        return [
            pltpu.make_async_remote_copy(
                src_ref=ins[a].at[target],
                dst_ref=outs[a].at[me],
                send_sem=send_sem.at[a, k],
                recv_sem=recv_sem.at[a, k],
                device_id=peer_id(axes, sizes, target),
                device_id_type=MESH,
            )
            for a in range(count)
        ]

    def push(i, carry):
        k = n // 2 + (1 - 2 * lax.rem(i, 2)) * lax.div(i + 1, 2)
        for copy in copies(k):
            copy.start()
        return carry

    lax.fori_loop(0, n - 1, push, 0)
    stores = [
        pltpu.make_async_copy(stages[a], outs[a].at[me], local_sem.at[a]) for a in range(count)
    ]
    for load in loads:
        load.wait()
    for store in stores:
        store.start()
    for store in stores:
        store.wait()

    def finish(k, carry):
        for copy in copies(k):
            copy.wait()
        return carry

    lax.fori_loop(1, n, finish, 0)


def exchange(arrays, axes, collective_id):
    sizes = [lax.axis_size(a) for a in axes]
    n = arrays[0].shape[0]
    count = len(arrays)
    moved = sum(a.size * 2 for a in arrays)
    return pl.pallas_call(
        functools.partial(exchange_kernel, axes, sizes, n, count),
        out_shape=[jax.ShapeDtypeStruct(a.shape, a.dtype) for a in arrays],
        in_specs=[pl.BlockSpec(memory_space=pl.ANY)] * count,
        out_specs=[pl.BlockSpec(memory_space=pl.ANY)] * count,
        scratch_shapes=[pltpu.VMEM(a.shape[1:], a.dtype) for a in arrays]
        + [
            pltpu.SemaphoreType.DMA((count, n)),
            pltpu.SemaphoreType.DMA((count, n)),
            pltpu.SemaphoreType.DMA((count,)),
        ],
        compiler_params=pltpu.CompilerParams(
            collective_id=collective_id, has_side_effects=True, vmem_limit_bytes=VMEM_LIMIT
        ),
        cost_estimate=pl.CostEstimate(flops=0, bytes_accessed=moved * 20, transcendentals=0),
    )(*arrays)


def attend_kernel(block, q_ref, k_ref, v_ref, out_ref):
    sources, _, rows, width = q_ref.shape
    length = sources * rows
    scale = width ** (-0.5)
    tri_row = lax.broadcasted_iota(jnp.int32, (block, block), 0)
    tri_col = lax.broadcasted_iota(jnp.int32, (block, block), 1)
    suffix_ones = (tri_row >= tri_col).astype(jnp.bfloat16)
    is_past = tri_col < tri_row
    per = block // rows

    def piece(ref, index):
        return ref[index * per : (index + 1) * per, 0].reshape(block, width)

    for q_block in range(length // block):
        query = piece(q_ref, q_block)
        total = jnp.zeros((block, width), jnp.float32)
        later = jnp.zeros((block, 1), jnp.float32)
        for k_block in range(q_block, -1, -1):
            scores = (
                lax.dot_general(
                    query,
                    piece(k_ref, k_block),
                    (((1,), (1,)), ((), ())),
                    preferred_element_type=jnp.float32,
                )
                * scale
            )
            soft = jnp.maximum(scores, 0.0) + jnp.log(1.0 + jnp.exp(-jnp.abs(scores)))
            if k_block == q_block:
                soft = jnp.where(is_past, soft, 0.0)
            high = soft.astype(jnp.bfloat16)
            low = (soft - high.astype(jnp.float32)).astype(jnp.bfloat16)
            suffix = jnp.dot(high, suffix_ones, preferred_element_type=jnp.float32) + jnp.dot(
                low, suffix_ones, preferred_element_type=jnp.float32
            )
            weights = jnp.exp(scores - suffix - later)
            if k_block == q_block:
                weights = jnp.where(is_past, weights, 0.0)
            total = total + jnp.dot(
                weights.astype(jnp.bfloat16),
                piece(v_ref, k_block),
                preferred_element_type=jnp.float32,
            )
            if k_block > 0:
                later = later + suffix[:, :1]
        out_ref[q_block * per : (q_block + 1) * per, 0] = total.astype(jnp.bfloat16).reshape(
            per, rows, width
        )


def attend(query, key, value):
    sources, heads, rows, width = query.shape
    block = rows * max(1, min(sources, 256 // rows))
    spec = pl.BlockSpec((sources, 1, rows, width), lambda h: (0, h, 0, 0))
    return pl.pallas_call(
        functools.partial(attend_kernel, block),
        grid=(heads,),
        out_shape=jax.ShapeDtypeStruct(query.shape, jnp.bfloat16),
        in_specs=[spec] * 3,
        out_specs=spec,
        compiler_params=pltpu.CompilerParams(vmem_limit_bytes=VMEM_LIMIT),
        cost_estimate=pl.CostEstimate(
            flops=6 * heads * (sources * rows) ** 2 * width, bytes_accessed=8 * query.size, transcendentals=0
        ),
    )(query, key, value)


def mix_kernel(steps, attn_ref, weight_ref, resid_ref, mixer_ref, expert_ref, pick_ref,
               stream_ref, *rest):
    sent_refs, projected = rest[:-1], rest[-1]
    step = pl.program_id(0)
    heads = attn_ref.shape[0]
    columns = weight_ref.shape[1]
    flat = jnp.concatenate([attn_ref[h] for h in range(heads)], axis=1)
    start = pl.multiple_of(step * columns, columns)
    projected[:, pl.ds(start, columns)] = jnp.dot(
        flat, weight_ref[...], preferred_element_type=jnp.float32
    )

    @pl.when(step == steps - 1)
    def _():
        stream = (
            resid_ref[...].astype(jnp.float32)
            + normed_token_rows(projected[...], mixer_ref[...])
        ).astype(jnp.bfloat16)
        stream_ref[...] = stream
        tokens = normed_token_rows(stream.astype(jnp.float32), expert_ref[...]).astype(jnp.bfloat16)
        row = 0
        for ref in sent_refs:
            many = ref.shape[0]
            ref[...] = jnp.dot(
                pick_ref[row : row + many], tokens, preferred_element_type=jnp.float32
            ).astype(jnp.bfloat16)
            row += many


def mix(attn, weight, residual, mixer_gain, expert_gain, pick, splits):
    heads, rows, width = attn.shape
    depth, features = weight.shape
    columns = min(1024, features)
    steps = features // columns
    whole = lambda shape: pl.BlockSpec(shape, lambda i: (0,) * len(shape))
    return pl.pallas_call(
        functools.partial(mix_kernel, steps),
        grid=(steps,),
        out_shape=[jax.ShapeDtypeStruct((many, features), jnp.bfloat16) for many in [rows] + splits],
        in_specs=[
            whole(attn.shape),
            pl.BlockSpec((depth, columns), lambda i: (0, i)),
            whole(residual.shape),
            whole((1, features)),
            whole((1, features)),
            whole(pick.shape),
        ],
        out_specs=[whole((many, features)) for many in [rows] + splits],
        scratch_shapes=[pltpu.VMEM((rows, features), jnp.float32)],
        compiler_params=pltpu.CompilerParams(vmem_limit_bytes=VMEM_LIMIT),
    )(attn, weight, residual, mixer_gain[None], expert_gain[None], pick)


def expert_kernel(count, *refs):
    ins, (gate_ref, up_ref, down_ref) = refs[:count], refs[count : count + 3]
    outs = refs[count + 3 :]
    for a in range(count):
        rows = ins[a][...]
        gate = jnp.dot(rows, gate_ref[...], preferred_element_type=jnp.float32)
        upward = jnp.dot(rows, up_ref[...], preferred_element_type=jnp.float32)
        hidden = (gate / (1.0 + jnp.exp(-gate)) * upward).astype(jnp.bfloat16)
        outs[a][...] = jnp.dot(
            hidden, down_ref[...], preferred_element_type=jnp.float32
        ).astype(jnp.bfloat16)


def serve(arrays, gate, up, down):
    return pl.pallas_call(
        functools.partial(expert_kernel, len(arrays)),
        out_shape=[jax.ShapeDtypeStruct(a.shape, a.dtype) for a in arrays],
        in_specs=[pl.BlockSpec(memory_space=pltpu.VMEM)] * (len(arrays) + 3),
        out_specs=[pl.BlockSpec(memory_space=pltpu.VMEM)] * len(arrays),
        compiler_params=pltpu.CompilerParams(vmem_limit_bytes=VMEM_LIMIT),
    )(*arrays, gate, up, down)


def combine_kernel(count, *refs):
    ins = refs[:count]
    high_ref, low_ref, stream_ref, gain_ref, out_ref = refs[count:]
    combined, row = 0.0, 0
    for ref in ins:
        many = ref.shape[0]
        for share in (high_ref, low_ref):
            combined = combined + jnp.dot(
                share[:, row : row + many], ref[...], preferred_element_type=jnp.float32
            )
        row += many
    out_ref[...] = (
        stream_ref[...].astype(jnp.float32) + normed_token_rows(combined, gain_ref[...])
    ).astype(jnp.bfloat16)


def combine(arrays, high, low, stream, gain):
    return pl.pallas_call(
        functools.partial(combine_kernel, len(arrays)),
        out_shape=jax.ShapeDtypeStruct(stream.shape, jnp.bfloat16),
        in_specs=[pl.BlockSpec(memory_space=pltpu.VMEM)] * (len(arrays) + 4),
        out_specs=pl.BlockSpec(memory_space=pltpu.VMEM),
        compiler_params=pltpu.CompilerParams(vmem_limit_bytes=VMEM_LIMIT),
    )(*arrays, high, low, stream, gain[None])


def local(
    queries,
    key_rows,
    values,
    residual,
    out_weight,
    mixer_gain,
    expert_gain,
    gate_weight,
    up_weight,
    expert_down_matrix,
    routes,
    route_weight,
    output_gain,
):
    full_weight = lax.all_gather(out_weight, "dp", axis=1, tiled=True)
    sp = lax.axis_size("sp")
    _, local_rows, heads, width = queries.shape
    features = residual.shape[2]

    def by_head(tensor):
        return jnp.transpose(tensor[0], (1, 0, 2)).reshape(sp, heads // sp, local_rows, width)

    head_parts = exchange([by_head(queries), by_head(key_rows), by_head(values)], ("sp",), 0)
    attended = attend(*head_parts)
    (token_parts,) = exchange([attended], ("sp",), 1)

    experts = sp * lax.axis_size("dp")
    top_count = routes.shape[2]
    capacity = max(2, 3 * local_rows // experts)
    picked = routes[0].reshape(local_rows * top_count)
    onehot = (
        picked[:, None] == lax.broadcasted_iota(jnp.int32, (picked.shape[0], experts), 1)
    ).astype(jnp.bfloat16)
    count = picked.shape[0]
    earlier = (
        lax.broadcasted_iota(jnp.int32, (count, count), 1)
        < lax.broadcasted_iota(jnp.int32, (count, count), 0)
    ).astype(jnp.bfloat16)
    before = jnp.dot(earlier, onehot, preferred_element_type=jnp.float32)
    rank = jnp.sum(before * onehot.astype(jnp.float32), axis=1).astype(jnp.int32)
    groups = [g for g in (capacity // 8 * 8, capacity % 8) if g]
    splits = [g * experts for g in groups]
    slot, first, base = jnp.full((count,), -1, jnp.int32), 0, 0
    for g in groups:
        inside = (rank >= first) & (rank < first + g)
        slot = jnp.where(inside, base + picked * g + rank - first, slot)
        first, base = first + g, base + g * experts
    slot = slot.reshape(local_rows, top_count)
    slot_ids = lax.broadcasted_iota(jnp.int32, (local_rows, base), 1)
    hits = [slot[:, k : k + 1] == slot_ids for k in range(top_count)]
    pick = functools.reduce(jnp.logical_or, hits).astype(jnp.bfloat16).T
    share = sum(jnp.where(hits[k], route_weight[0][:, k : k + 1], 0.0) for k in range(top_count))
    share_high = share.astype(jnp.bfloat16)
    share_low = (share - share_high.astype(jnp.float32)).astype(jnp.bfloat16)

    stream, *outgoing = mix(
        token_parts.reshape(heads, local_rows, width),
        full_weight,
        residual[0],
        mixer_gain,
        expert_gain,
        pick,
        splits,
    )

    def blocks(arrays):
        return [a.reshape(experts, g, features) for a, g in zip(arrays, groups)]

    def flat(arrays):
        return [a.reshape(-1, features) for a in arrays]

    arrived = exchange(blocks(outgoing), ("sp", "dp"), 2)
    results = serve(flat(arrived), gate_weight[0], up_weight[0], expert_down_matrix[0])
    returned = exchange(blocks(results), ("sp", "dp"), 3)
    output = combine(flat(returned), share_high, share_low, stream, output_gain)
    return output[None]


def solution(mesh):
    in_specs = (
        P("dp", "sp", None, None),
        P("dp", "sp", None, None),
        P("dp", "sp", None, None),
        P("dp", "sp", None),
        P(None, "dp"),
        P(),
        P(),
        P(("sp", "dp"), None, None),
        P(("sp", "dp"), None, None),
        P(("sp", "dp"), None, None),
        P("dp", "sp", None),
        P("dp", "sp", None),
        P(),
    )
    out_specs = P("dp", "sp", None)
    return jax.shard_map(local, mesh=mesh, in_specs=in_specs, out_specs=out_specs, check_vma=False)
```

```python
import functools

import jax
import jax.numpy as jnp
from jax import lax
from jax.experimental import pallas as pl
from jax.experimental.pallas import tpu as pltpu
from jax.sharding import PartitionSpec as P

EPSILON = 1e-06
MESH = pl.DeviceIdType.MESH
VMEM_LIMIT = 56 * 1024 * 1024


def normed_token_rows(matrix, gain):
    return matrix * lax.rsqrt(jnp.mean(matrix * matrix, axis=-1, keepdims=True) + EPSILON) * gain


def peer_id(axes, sizes, flat):
    if len(axes) == 1:
        return {axes[0]: flat}
    return {axes[0]: lax.div(flat, sizes[1]), axes[1]: lax.rem(flat, sizes[1])}


def exchange_kernel(axes, sizes, n, count, *refs):
    ins, outs = refs[:count], refs[count : 2 * count]
    stages = refs[2 * count : 3 * count]
    send_sem, recv_sem, local_sem = refs[3 * count :]
    me = lax.axis_index(axes[0])
    if len(axes) == 2:
        me = me * sizes[1] + lax.axis_index(axes[1])

    barrier = pltpu.get_barrier_semaphore()

    def greet(k, carry):
        pl.semaphore_signal(
            barrier, inc=1, device_id=peer_id(axes, sizes, lax.rem(me + k, n)), device_id_type=MESH
        )
        return carry

    lax.fori_loop(1, n, greet, 0)
    loads = [
        pltpu.make_async_copy(ins[a].at[me], stages[a], local_sem.at[a]) for a in range(count)
    ]
    for load in loads:
        load.start()
    pl.semaphore_wait(barrier, n - 1)

    def copies(k):
        target = lax.rem(me + k, n)
        return [
            pltpu.make_async_remote_copy(
                src_ref=ins[a].at[target],
                dst_ref=outs[a].at[me],
                send_sem=send_sem.at[a, k],
                recv_sem=recv_sem.at[a, k],
                device_id=peer_id(axes, sizes, target),
                device_id_type=MESH,
            )
            for a in range(count)
        ]

    def push(i, carry):
        k = n // 2 + (1 - 2 * lax.rem(i, 2)) * lax.div(i + 1, 2)
        for copy in copies(k):
            copy.start()
        return carry

    lax.fori_loop(0, n - 1, push, 0)
    stores = [
        pltpu.make_async_copy(stages[a], outs[a].at[me], local_sem.at[a]) for a in range(count)
    ]
    for load in loads:
        load.wait()
    for store in stores:
        store.start()
    for store in stores:
        store.wait()

    def finish(k, carry):
        for copy in copies(k):
            copy.wait()
        return carry

    lax.fori_loop(1, n, finish, 0)


def exchange(arrays, axes, collective_id):
    sizes = [lax.axis_size(a) for a in axes]
    n = arrays[0].shape[0]
    count = len(arrays)
    moved = sum(a.size * 2 for a in arrays)
    return pl.pallas_call(
        functools.partial(exchange_kernel, axes, sizes, n, count),
        out_shape=[jax.ShapeDtypeStruct(a.shape, a.dtype) for a in arrays],
        in_specs=[pl.BlockSpec(memory_space=pl.ANY)] * count,
        out_specs=[pl.BlockSpec(memory_space=pl.ANY)] * count,
        scratch_shapes=[pltpu.VMEM(a.shape[1:], a.dtype) for a in arrays]
        + [
            pltpu.SemaphoreType.DMA((count, n)),
            pltpu.SemaphoreType.DMA((count, n)),
            pltpu.SemaphoreType.DMA((count,)),
        ],
        compiler_params=pltpu.CompilerParams(
            collective_id=collective_id, has_side_effects=True, vmem_limit_bytes=VMEM_LIMIT
        ),
        cost_estimate=pl.CostEstimate(flops=0, bytes_accessed=moved * 20, transcendentals=0),
    )(*arrays)


def attend_kernel(block, q_ref, k_ref, v_ref, out_ref):
    sources, _, rows, width = q_ref.shape
    length = sources * rows
    scale = width ** (-0.5)
    tri_row = lax.broadcasted_iota(jnp.int32, (block, block), 0)
    tri_col = lax.broadcasted_iota(jnp.int32, (block, block), 1)
    suffix_ones = (tri_row >= tri_col).astype(jnp.bfloat16)
    is_past = tri_col < tri_row
    per = block // rows

    def piece(ref, index):
        return ref[index * per : (index + 1) * per, 0].reshape(block, width)

    for q_block in range(length // block):
        query = piece(q_ref, q_block)
        total = jnp.zeros((block, width), jnp.float32)
        later = jnp.zeros((block, 1), jnp.float32)
        for k_block in range(q_block, -1, -1):
            scores = (
                lax.dot_general(
                    query,
                    piece(k_ref, k_block),
                    (((1,), (1,)), ((), ())),
                    preferred_element_type=jnp.float32,
                )
                * scale
            )
            soft = jnp.maximum(scores, 0.0) + jnp.log(1.0 + jnp.exp(-jnp.abs(scores)))
            if k_block == q_block:
                soft = jnp.where(is_past, soft, 0.0)
            high = soft.astype(jnp.bfloat16)
            low = (soft - high.astype(jnp.float32)).astype(jnp.bfloat16)
            suffix = jnp.dot(high, suffix_ones, preferred_element_type=jnp.float32) + jnp.dot(
                low, suffix_ones, preferred_element_type=jnp.float32
            )
            weights = jnp.exp(scores - suffix - later)
            if k_block == q_block:
                weights = jnp.where(is_past, weights, 0.0)
            total = total + jnp.dot(
                weights.astype(jnp.bfloat16),
                piece(v_ref, k_block),
                preferred_element_type=jnp.float32,
            )
            if k_block > 0:
                later = later + suffix[:, :1]
        out_ref[q_block * per : (q_block + 1) * per, 0] = total.astype(jnp.bfloat16).reshape(
            per, rows, width
        )


def attend(query, key, value):
    sources, heads, rows, width = query.shape
    block = rows * max(1, min(sources, 256 // rows))
    spec = pl.BlockSpec((sources, 1, rows, width), lambda h: (0, h, 0, 0))
    return pl.pallas_call(
        functools.partial(attend_kernel, block),
        grid=(heads,),
        out_shape=jax.ShapeDtypeStruct(query.shape, jnp.bfloat16),
        in_specs=[spec] * 3,
        out_specs=spec,
        compiler_params=pltpu.CompilerParams(vmem_limit_bytes=VMEM_LIMIT),
        cost_estimate=pl.CostEstimate(
            flops=6 * heads * (sources * rows) ** 2 * width, bytes_accessed=8 * query.size, transcendentals=0
        ),
    )(query, key, value)


def project_kernel(attn_ref, weight_ref, out_ref):
    for part in range(attn_ref.shape[0]):
        flat = jnp.concatenate([attn_ref[part, h] for h in range(attn_ref.shape[1])], axis=1)
        out_ref[part] = jnp.dot(
            flat, weight_ref[...], preferred_element_type=jnp.float32
        ).astype(jnp.bfloat16)


def project(attn, weight):
    parts, _, rows, _ = attn.shape
    return pl.pallas_call(
        project_kernel,
        out_shape=jax.ShapeDtypeStruct((parts, rows, weight.shape[1]), jnp.bfloat16),
        in_specs=[pl.BlockSpec(memory_space=pltpu.VMEM)] * 2,
        out_specs=pl.BlockSpec(memory_space=pltpu.VMEM),
        compiler_params=pltpu.CompilerParams(vmem_limit_bytes=VMEM_LIMIT),
    )(attn, weight)


def mix_kernel(parts_ref, resid_ref, mixer_ref, expert_ref, pick_ref, stream_ref, *sent_refs):
    projected = jnp.concatenate(
        [parts_ref[part].astype(jnp.float32) for part in range(parts_ref.shape[0])], axis=1
    )
    stream = (
        resid_ref[...].astype(jnp.float32) + normed_token_rows(projected, mixer_ref[...])
    ).astype(jnp.bfloat16)
    stream_ref[...] = stream
    tokens = normed_token_rows(stream.astype(jnp.float32), expert_ref[...]).astype(jnp.bfloat16)
    row = 0
    for ref in sent_refs:
        many = ref.shape[0]
        ref[...] = jnp.dot(
            pick_ref[row : row + many], tokens, preferred_element_type=jnp.float32
        ).astype(jnp.bfloat16)
        row += many


def mix(parts, residual, mixer_gain, expert_gain, pick, splits):
    rows, features = residual.shape
    return pl.pallas_call(
        mix_kernel,
        out_shape=[jax.ShapeDtypeStruct((many, features), jnp.bfloat16) for many in [rows] + splits],
        in_specs=[pl.BlockSpec(memory_space=pltpu.VMEM)] * 5,
        out_specs=[pl.BlockSpec(memory_space=pltpu.VMEM)] * (1 + len(splits)),
        compiler_params=pltpu.CompilerParams(vmem_limit_bytes=VMEM_LIMIT),
    )(parts, residual, mixer_gain[None], expert_gain[None], pick)


def expert_kernel(count, *refs):
    ins, (gate_ref, up_ref, down_ref) = refs[:count], refs[count : count + 3]
    outs = refs[count + 3 :]
    for a in range(count):
        rows = ins[a][...]
        gate = jnp.dot(rows, gate_ref[...], preferred_element_type=jnp.float32)
        upward = jnp.dot(rows, up_ref[...], preferred_element_type=jnp.float32)
        hidden = (gate / (1.0 + jnp.exp(-gate)) * upward).astype(jnp.bfloat16)
        outs[a][...] = jnp.dot(
            hidden, down_ref[...], preferred_element_type=jnp.float32
        ).astype(jnp.bfloat16)


def serve(arrays, gate, up, down):
    return pl.pallas_call(
        functools.partial(expert_kernel, len(arrays)),
        out_shape=[jax.ShapeDtypeStruct(a.shape, a.dtype) for a in arrays],
        in_specs=[pl.BlockSpec(memory_space=pltpu.VMEM)] * (len(arrays) + 3),
        out_specs=[pl.BlockSpec(memory_space=pltpu.VMEM)] * len(arrays),
        compiler_params=pltpu.CompilerParams(vmem_limit_bytes=VMEM_LIMIT),
    )(*arrays, gate, up, down)


def combine_kernel(count, *refs):
    ins = refs[:count]
    high_ref, low_ref, stream_ref, gain_ref, out_ref = refs[count:]
    combined, row = 0.0, 0
    for ref in ins:
        many = ref.shape[0]
        for share in (high_ref, low_ref):
            combined = combined + jnp.dot(
                share[:, row : row + many], ref[...], preferred_element_type=jnp.float32
            )
        row += many
    out_ref[...] = (
        stream_ref[...].astype(jnp.float32) + normed_token_rows(combined, gain_ref[...])
    ).astype(jnp.bfloat16)


def combine(arrays, high, low, stream, gain):
    return pl.pallas_call(
        functools.partial(combine_kernel, len(arrays)),
        out_shape=jax.ShapeDtypeStruct(stream.shape, jnp.bfloat16),
        in_specs=[pl.BlockSpec(memory_space=pltpu.VMEM)] * (len(arrays) + 4),
        out_specs=pl.BlockSpec(memory_space=pltpu.VMEM),
        compiler_params=pltpu.CompilerParams(vmem_limit_bytes=VMEM_LIMIT),
    )(*arrays, high, low, stream, gain[None])


def local(
    queries,
    key_rows,
    values,
    residual,
    out_weight,
    mixer_gain,
    expert_gain,
    gate_weight,
    up_weight,
    expert_down_matrix,
    routes,
    route_weight,
    output_gain,
):
    sp = lax.axis_size("sp")
    _, local_rows, heads, width = queries.shape
    features = residual.shape[2]

    def by_head(tensor):
        return jnp.transpose(tensor[0], (1, 0, 2)).reshape(sp, heads // sp, local_rows, width)

    head_parts = exchange([by_head(queries), by_head(key_rows), by_head(values)], ("sp",), 0)
    attended = attend(*head_parts)
    (token_parts,) = exchange([attended], ("sp",), 1)

    dp = lax.axis_size("dp")
    token_heads = token_parts.reshape(heads, local_rows, width)
    (group_heads,) = exchange([jnp.broadcast_to(token_heads[None], (dp,) + token_heads.shape)], ("dp",), 4)
    (projected_parts,) = exchange([project(group_heads, out_weight)], ("dp",), 5)

    experts = sp * dp
    top_count = routes.shape[2]
    capacity = max(2, 3 * local_rows // experts)
    picked = routes[0].reshape(local_rows * top_count)
    onehot = (
        picked[:, None] == lax.broadcasted_iota(jnp.int32, (picked.shape[0], experts), 1)
    ).astype(jnp.bfloat16)
    count = picked.shape[0]
    earlier = (
        lax.broadcasted_iota(jnp.int32, (count, count), 1)
        < lax.broadcasted_iota(jnp.int32, (count, count), 0)
    ).astype(jnp.bfloat16)
    before = jnp.dot(earlier, onehot, preferred_element_type=jnp.float32)
    rank = jnp.sum(before * onehot.astype(jnp.float32), axis=1).astype(jnp.int32)
    groups = [g for g in (capacity // 8 * 8, capacity % 8) if g]
    splits = [g * experts for g in groups]
    slot, first, base = jnp.full((count,), -1, jnp.int32), 0, 0
    for g in groups:
        inside = (rank >= first) & (rank < first + g)
        slot = jnp.where(inside, base + picked * g + rank - first, slot)
        first, base = first + g, base + g * experts
    slot = slot.reshape(local_rows, top_count)
    slot_ids = lax.broadcasted_iota(jnp.int32, (local_rows, base), 1)
    hits = [slot[:, k : k + 1] == slot_ids for k in range(top_count)]
    pick = functools.reduce(jnp.logical_or, hits).astype(jnp.bfloat16).T
    share = sum(jnp.where(hits[k], route_weight[0][:, k : k + 1], 0.0) for k in range(top_count))
    share_high = share.astype(jnp.bfloat16)
    share_low = (share - share_high.astype(jnp.float32)).astype(jnp.bfloat16)

    stream, *outgoing = mix(
        projected_parts,
        residual[0],
        mixer_gain,
        expert_gain,
        pick,
        splits,
    )

    def blocks(arrays):
        return [a.reshape(experts, g, features) for a, g in zip(arrays, groups)]

    def flat(arrays):
        return [a.reshape(-1, features) for a in arrays]

    arrived = exchange(blocks(outgoing), ("sp", "dp"), 2)
    results = serve(flat(arrived), gate_weight[0], up_weight[0], expert_down_matrix[0])
    returned = exchange(blocks(results), ("sp", "dp"), 3)
    output = combine(flat(returned), share_high, share_low, stream, output_gain)
    return output[None]


def solution(mesh):
    in_specs = (
        P("dp", "sp", None, None),
        P("dp", "sp", None, None),
        P("dp", "sp", None, None),
        P("dp", "sp", None),
        P(None, "dp"),
        P(),
        P(),
        P(("sp", "dp"), None, None),
        P(("sp", "dp"), None, None),
        P(("sp", "dp"), None, None),
        P("dp", "sp", None),
        P("dp", "sp", None),
        P(),
    )
    out_specs = P("dp", "sp", None)
    return jax.shard_map(local, mesh=mesh, in_specs=in_specs, out_specs=out_specs, check_vma=False)
```
